512 devices in a mesh: sp: 128 (over z, x, core), tp: 4 (over y).
Axes of the slice: x: 4, y: 4, z: 16, core: 2. Of those that a mesh axis runs over, the one named last changes fastest.
Arguments:
- tokens: bfloat16 [16384, 1024], P(('sp', 'tp')), may hold values from -13 to 13, as said below
- norm_gain: float32 [1024], replicated, may hold values from 0.5 to 1.5
- query_weight: bfloat16 [1024, 4096], P(None, 'tp'), may hold values from -0.1875 to 0.1875
- key_weight: bfloat16 [1024, 512], P(None, 'tp'), may hold values from -0.1875 to 0.1875
- value_weight: bfloat16 [1024, 512], P(None, 'tp'), may hold values from -0.1875 to 0.1875
- query_gain: float32 [128], replicated, may hold values from 0.5 to 1.5
- key_gain: float32 [128], replicated, may hold values from 0.5 to 1.5
- output_weight: bfloat16 [4096, 1024], P('tp'), may hold values from -1 to 1
Outputs:
- mixed: bfloat16 [16384, 1024], P(('sp', 'tp'))
The draws below stay inside these ranges and needn't reach their ends.
Inputs may be any that keep to these rules, and one draw needn't show every extreme that they name: Every entry of tokens lies between -13 and 13.
All inputs are finite; a program needn't handle non-finite values.
Results may differ from the reference program's by a relative error of at most 0.015.
Values may be sent and summed in bfloat16 or wider, within the bound.
A program may use at most 64 MiB of HBM per device.

```python
import jax
import jax.numpy as jnp
from jax import lax

D = 1024
HEADS = 32
KV_HEADS = 4
HEAD_DIM = 128
GRID_W = 64
TOK_SP = 128
TOKENS = 16384


def draw_tokens(key, part):
    noise_key = jax.random.fold_in(key, 11)
    region_key = jax.random.fold_in(key, 12)
    regions = TOKENS // TOK_SP
    noise_part = jnp.clip(jax.random.normal(noise_key, (TOKENS, D), jnp.float32), -4.0, 4.0)
    centres = 1.5 * jnp.clip(jax.random.normal(region_key, (regions, D), jnp.float32), -3.0, 3.0)
    spread_means = jnp.broadcast_to(centres[:, None, :], (regions, TOK_SP, D)).reshape(TOKENS, D)
    return (noise_part + spread_means).astype(jnp.bfloat16)


def shard_levels(stream_key, extent, cuts, smallest, largest):
    level = 1.0
    for dim, blocks in cuts:
        steps = jax.random.uniform(jax.random.fold_in(jax.random.fold_in(stream_key, 6), dim), (blocks,), jnp.float32, smallest / len(cuts), largest / len(cuts))
        level = level * jnp.repeat(jnp.exp(steps), extent[dim] // blocks).reshape((-1,) + (1,) * (len(extent) - 1 - dim))
    return level


def centred(key, extent, deviation, limit, shards=(), held_as=jnp.bfloat16):
    array = deviation * jax.random.normal(key, extent, jnp.float32)
    if shards:
        array = array * shard_levels(key, extent, shards, -0.22, 0.18)
    return jnp.clip(array, -limit, limit).astype(held_as)


def setup_inputs(seed: int = 0) -> dict:
    key_list = jax.random.split(jax.random.key(seed), 9)
    tokens = draw_tokens(jax.random.fold_in(key_list[8], 71), 0)
    norm_gain = jnp.clip(1.0 + 0.1 * jax.random.normal(key_list[1], (D,), jnp.float32), 0.5, 1.5)
    query_weight = centred(key_list[2], (D, HEADS * HEAD_DIM), D ** -0.5, 0.1875, ((1, 4),))
    key_weight = centred(key_list[3], (D, KV_HEADS * HEAD_DIM), D ** -0.5, 0.1875, ((1, 4),))
    value_weight = centred(key_list[4], (D, KV_HEADS * HEAD_DIM), D ** -0.5, 0.1875, ((1, 4),))
    query_gain = jnp.clip(1.0 + 0.1 * jax.random.normal(key_list[5], (HEAD_DIM,), jnp.float32), 0.5, 1.5)
    key_gain = jnp.clip(1.0 + 0.1 * jax.random.normal(key_list[6], (HEAD_DIM,), jnp.float32), 0.5, 1.5)
    output_weight = centred(key_list[7], (HEADS * HEAD_DIM, D), (HEADS * HEAD_DIM * TOK_SP // TOKENS) ** -0.5, 1.0, ((0, 4),))
    return dict(tokens=tokens, norm_gain=norm_gain, query_weight=query_weight, key_weight=key_weight, value_weight=value_weight, query_gain=query_gain, key_gain=key_gain, output_weight=output_weight)


epsilon = 1e-06
rotary_base = 10000.0

def rotation_tables(first_position, length, head_dim):
    positions = first_position + lax.iota(jnp.int32, length)
    grid_row = (positions // GRID_W).astype(jnp.float32)
    grid_column = (positions % GRID_W).astype(jnp.float32)
    axis_dim = head_dim // 2
    frequencies = rotary_base ** (-jnp.arange(0, axis_dim, 2, dtype=jnp.float32) / axis_dim)
    angles = jnp.concatenate([grid_row[:, None] * frequencies[None, :], grid_column[:, None] * frequencies[None, :]], axis=-1)
    return (jnp.cos(angles), jnp.sin(angles))

def normalize_rotate(projected, gain, cosine, sine):
    widened = projected.astype(jnp.float32)
    scaled = widened * lax.rsqrt(lax.optimization_barrier(jnp.mean(widened * widened, axis=-1, keepdims=True)) + epsilon) * gain.astype(jnp.float32)
    paired = scaled.reshape(scaled.shape[:-1] + (scaled.shape[-1] // 2, 2))
    even_half = paired[..., 0]
    odd_half = paired[..., 1]
    cosine_rows = cosine[:, None, :]
    sine_rows = sine[:, None, :]
    turned = jnp.stack([even_half * cosine_rows - odd_half * sine_rows, even_half * sine_rows + odd_half * cosine_rows], axis=-1)
    return turned.reshape(projected.shape).astype(jnp.bfloat16)

def rms_rows(tokens, norm_gain):
    widened = tokens.astype(jnp.float32)
    scaled = widened * lax.rsqrt(lax.optimization_barrier(jnp.mean(widened * widened, axis=-1, keepdims=True)) + epsilon)
    return (scaled * norm_gain.astype(jnp.float32)).astype(jnp.bfloat16)

def reference(tokens, norm_gain, query_weight, key_weight, value_weight, query_gain, key_gain, output_weight):
    normed = rms_rows(tokens, norm_gain)
    query_part = jnp.dot(normed, query_weight, preferred_element_type=jnp.float32).astype(jnp.bfloat16)
    key_part = jnp.dot(normed, key_weight, preferred_element_type=jnp.float32).astype(jnp.bfloat16)
    value_part = jnp.dot(normed, value_weight, preferred_element_type=jnp.float32).astype(jnp.bfloat16)
    cosine, sine = rotation_tables(0, TOKENS, HEAD_DIM)
    queries = normalize_rotate(query_part.reshape(TOKENS, HEADS, HEAD_DIM), query_gain, cosine, sine)
    keys = normalize_rotate(key_part.reshape(TOKENS, KV_HEADS, HEAD_DIM), key_gain, cosine, sine)
    key_all = keys.astype(jnp.float32)
    value_all = value_part.reshape(TOKENS, KV_HEADS, HEAD_DIM).astype(jnp.float32)
    group_size = HEADS // KV_HEADS
    block_count = TOKENS // GRID_W
    query_blocks = queries.reshape(block_count, GRID_W, KV_HEADS, group_size, HEAD_DIM)
    scale = HEAD_DIM ** (-0.5)

    def one_block(query_block):
        scores = jnp.einsum('qkgd,skd->kgqs', query_block.astype(jnp.float32), key_all, precision=lax.Precision.HIGHEST) * scale
        highest = lax.optimization_barrier(jnp.max(scores, axis=-1, keepdims=True))
        weights = jnp.exp(scores - highest)
        denominator = lax.optimization_barrier(jnp.sum(weights, axis=-1))
        rounded = lax.optimization_barrier(weights.astype(jnp.bfloat16)).astype(jnp.float32)
        numerator = jnp.einsum('kgqs,skd->kgqd', rounded, value_all, precision=lax.Precision.HIGHEST)
        return (numerator / denominator[..., None]).astype(jnp.bfloat16)
    attended = lax.map(one_block, query_blocks)
    attended = attended.transpose(0, 3, 1, 2, 4).reshape(TOKENS, HEADS * HEAD_DIM)
    return jnp.dot(attended, output_weight, preferred_element_type=jnp.float32).astype(jnp.bfloat16)
```

```python
import functools
import math

import jax
import jax.numpy as jnp
import numpy as np
from jax import lax
from jax.experimental import pallas as pl
from jax.experimental.pallas import tpu as pltpu
from jax.sharding import PartitionSpec as P

GRID_W = 64
EPS = 1e-06
ROTARY_BASE = 10000.0
HD = 128
BLK = 128
XN = 4
YN = 4
CUT = 96
HALF = (256 - CUT) // 2
MESH = pl.DeviceIdType.MESH
F32 = jnp.float32
BF16 = jnp.bfloat16


def position_tables(blocks):
    axis_dim = HD // 2
    freq = (ROTARY_BASE ** (-np.arange(0, axis_dim, 2, dtype=np.float32) / np.float32(axis_dim))).astype(np.float32)

    def pair(angles):
        cosine = np.repeat(np.cos(angles.astype(np.float64)), 2, axis=-1)
        sine = np.repeat(np.sin(angles.astype(np.float64)), 2, axis=-1)
        sine[..., 0::2] *= -1.0
        return cosine.astype(np.float32), sine.astype(np.float32)

    rows_in = BLK // GRID_W
    grid_rows = np.arange(blocks * rows_in, dtype=np.float32)
    rc, rs = pair(grid_rows[:, None] * freq[None, :])
    row_table = np.zeros((blocks, 8, HD), np.float32)
    row_table[:, 0:2, 0:axis_dim] = rc.reshape(blocks, rows_in, axis_dim)
    row_table[:, 2:4, 0:axis_dim] = rs.reshape(blocks, rows_in, axis_dim)
    columns = (np.arange(BLK) % GRID_W).astype(np.float32)
    cc, cs = pair(columns[:, None] * freq[None, :])
    col_table = np.zeros((2, BLK, HD), np.float32)
    col_table[0, :, axis_dim:] = cc
    col_table[1, :, axis_dim:] = cs
    return row_table, col_table


def layer_kernel(
    zn, tok_h, ngain_h, wq_h, wk_h, wv_h, qgain_h, kgain_h, wo_h, rtab_h, ctab_h, out_ref,
    tok_v, ngain_v, wq_v, wk_v, wv_v, qgain_v, kgain_v, wo_v, rtab_v, ctab_v,
    nbuf, kv, qt, acc, accr, mf, mbuf, rbuf,
    lsem, ysend, yrecv, y2send, y2recv, asend, arecv,
    zps, zpr, zms, zmr, xs, xr, qsem, esem,
):
    me = lax.axis_index("sp")
    yy = lax.axis_index("tp")
    core = lax.rem(me, 2)
    xx = lax.rem(me // 2, XN)
    zz = me // (2 * XN)
    steps = zn // 2

    def at(z, x, c, y):
        return ((z * XN + x) * 2 + c, y)

    def zrow(d):
        return lax.rem(zz + d + zn, zn)

    x_right = lax.rem(xx + 1, XN)
    x_left = lax.rem(xx + XN - 1, XN)
    x_far = lax.rem(xx + 2, XN)
    to_right = at(zz, x_right, core, yy)
    to_left = at(zz, x_left, core, yy)
    to_far = at(zz, x_far, core, yy)
    to_up = at(zrow(1), xx, core, yy)
    to_down = at(zrow(-1), xx, core, yy)
    partner = at(zz, xx, 1 - core, yy)

    def ypeer(d):
        return at(zz, xx, core, lax.rem(yy + d, YN))

    local = []
    for i, (src, dst) in enumerate((
        (tok_h, tok_v), (ngain_h, ngain_v), (wk_h, wk_v), (wv_h, wv_v), (wq_h, wq_v),
        (qgain_h, qgain_v), (kgain_h, kgain_v), (rtab_h.at[me], rtab_v), (ctab_h, ctab_v), (wo_h, wo_v),
    )):
        local.append(pltpu.make_async_copy(src, dst, lsem.at[i]))
    for copy in local:
        copy.start()

    barrier = pltpu.get_barrier_semaphore()
    peers = [to_right, to_left, to_far, to_up, to_down, partner] + [ypeer(d) for d in (1, 2, 3)]
    for peer in peers:
        pl.semaphore_signal(barrier, inc=1, device_id=peer, device_id_type=MESH)

    local[0].wait()
    local[1].wait()
    wide = tok_v[...].astype(F32)
    inv = lax.rsqrt(jnp.mean(wide * wide, axis=-1, keepdims=True) + EPS)
    nbuf[yy] = (wide * inv * ngain_v[...]).astype(BF16)
    acc[...] = jnp.zeros_like(acc)
    pl.semaphore_wait(barrier, len(peers))

    def rcopy(src, dst, ssem, rsem, device):
        return pltpu.make_async_remote_copy(
            src_ref=src, dst_ref=dst, send_sem=ssem, recv_sem=rsem, device_id=device, device_id_type=MESH)

    for d in (1, 2, 3):
        rcopy(nbuf.at[yy], nbuf.at[yy], ysend.at[d - 1], yrecv.at[d - 1], ypeer(d)).start()
    for i in range(2, 9):
        local[i].wait()

    token = lax.broadcasted_iota(jnp.int32, (BLK, HD), 0)
    lane = lax.broadcasted_iota(jnp.int32, (BLK, HD), 1)
    first = token < GRID_W
    even = lax.rem(lane, 2) == 0
    cosine = ctab_v[0] + jnp.where(first, rtab_v[0:1, :], rtab_v[1:2, :])
    sine = ctab_v[1] + jnp.where(first, rtab_v[2:3, :], rtab_v[3:4, :])

    def swapped(a):
        return jnp.where(even, pltpu.roll(a, HD - 1, 1), pltpu.roll(a, 1, 1))

    def tables(gain_ref, factor):
        gain = jnp.broadcast_to(gain_ref[...], (BLK, HD)) * factor
        return cosine * gain, sine * swapped(gain)

    def normalize_rotate(projected, tabs):
        wide = projected.astype(F32)
        inv = lax.rsqrt(jnp.mean(wide * wide, axis=-1, keepdims=True) + EPS)
        return (wide * tabs[0] + swapped(wide) * tabs[1]) * inv

    for d in (1, 2, 3):
        slot = nbuf.at[lax.rem(yy - d + YN, YN)]
        rcopy(slot, slot, ysend.at[d - 1], yrecv.at[d - 1], ypeer(d)).wait_recv()
    normed = nbuf[...].reshape(BLK, nbuf.shape[2])
    key_part = jnp.dot(normed, wk_v[...], preferred_element_type=F32).astype(BF16)
    value_part = jnp.dot(normed, wv_v[...], preferred_element_type=F32).astype(BF16)
    kv[zz, xx, 0:BLK, :] = normalize_rotate(key_part, tables(kgain_v, 1.0)).astype(BF16)
    kv[zz, xx, BLK:, :] = jnp.transpose(value_part.astype(F32)).astype(BF16)

    B = pl.ds(CUT, 256 - CUT)
    A = pl.ds(0, CUT)
    B1 = pl.ds(CUT, HALF)
    B2 = pl.ds(CUT + HALF, HALF)

    def zpart(row, k):
        if k == 0:
            return kv.at[row, xx, B]
        return kv.at[row, pl.ds(2 * (k - 1), 2), A]

    def up(s, k):
        part = zpart(zrow(-s), k)
        return rcopy(part, part, zps.at[s, k], zpr.at[s + 1, k], to_up)

    def down(s, k):
        part = zpart(zrow(s), k)
        return rcopy(part, part, zms.at[s, k], zmr.at[s + 1, k], to_down)

    def got_up(s, k):
        part = zpart(zrow(-s), k)
        rcopy(part, part, zps.at[0, k], zpr.at[s, k], to_up).wait_recv()

    def got_down(s, k):
        part = zpart(zrow(s), k)
        rcopy(part, part, zms.at[0, k], zmr.at[s, k], to_down).wait_recv()

    def across(row, j, i):
        part, device = (
            (kv.at[row, xx, B], to_right), (kv.at[row, xx, B], to_left),
            (kv.at[row, x_left, B1], to_right), (kv.at[row, x_right, B2], to_left),
        )[i]
        return rcopy(part, part, xs.at[j, i], xr.at[j, i], device)

    def got_across(row, j, i):
        part = (kv.at[row, x_left, B], kv.at[row, x_right, B], kv.at[row, x_far, B1], kv.at[row, x_far, B2])[i]
        rcopy(part, part, xs.at[j, i], xr.at[j, i], to_right).wait_recv()

    up(0, 0).start()
    down(0, 0).start()
    own_a = kv.at[zz, xx, A]
    a_sends = [
        rcopy(own_a, own_a, asend.at[0], arecv.at[0], to_right),
        rcopy(own_a, own_a, asend.at[1], arecv.at[1], to_left),
        rcopy(own_a, own_a, asend.at[2], arecv.at[2], to_far),
    ]
    for copy in a_sends:
        copy.start()
    across(zz, 0, 0).start()
    across(zz, 0, 1).start()

    query_part = jnp.dot(normed, wq_v[...], preferred_element_type=F32).astype(BF16)
    qtabs = tables(qgain_v, HD ** -0.5 * math.log2(math.e))
    heads = query_part.shape[1] // HD
    for h in range(heads):
        turned = normalize_rotate(query_part[:, h * HD:(h + 1) * HD], qtabs)
        qt[core, :, h * HD:(h + 1) * HD] = jnp.transpose(turned).astype(BF16)
    q_send = rcopy(qt.at[core], qt.at[core], qsem.at[0], qsem.at[1], partner)
    q_send.start()

    for i, column in enumerate((x_left, x_right, x_far)):
        part = kv.at[zz, column, A]
        rcopy(part, part, asend.at[i], arecv.at[i], to_right).wait_recv()
    for k in (1, 2):
        up(0, k).start()
        down(0, k).start()

    def fold_row(row):
        keys = jnp.concatenate([kv[row, i, 0:BLK, :] for i in range(XN)], axis=0)
        values = jnp.concatenate([kv[row, i, BLK:, :] for i in range(XN)], axis=1)

        @pl.loop(0, 2)
        def _(t):
            scores = jnp.dot(keys, qt[t], preferred_element_type=F32)
            weights = jnp.exp2(scores)
            acc[t, HD:, :] += weights.reshape(XN * BLK // 8, 8, qt.shape[2]).sum(0)
            acc[t, 0:HD, :] += jnp.dot(values, weights.astype(BF16), preferred_element_type=F32)

    def start_across(row, j):
        across(row, j, 0).start()
        across(row, j, 1).start()

    def relay_across(row, j):
        got_across(row, j, 0)
        across(row, j, 2).start()
        got_across(row, j, 1)
        across(row, j, 3).start()

    def finish_row(row, j):
        got_across(row, j, 2)
        got_across(row, j, 3)
        fold_row(row)

    def arrivals(s, k, last_up=False, last_down=False, has_down=True):
        got_up(s, k)
        if not last_up:
            up(s, k).start()
        if k == 0:
            start_across(zrow(-s), 2 * s - 1)
        if has_down:
            got_down(s, k)
            if not last_down:
                down(s, k).start()
            if k == 0:
                start_across(zrow(s), 2 * s)

    arrivals(1, 0)
    relay_across(zz, 0)
    arrivals(1, 1)
    arrivals(1, 2)
    qrecv = qt.at[1 - core]
    rcopy(qrecv, qrecv, qsem.at[0], qsem.at[1], partner).wait_recv()

    arrivals(2, 0)
    relay_across(zrow(-1), 1)
    relay_across(zrow(1), 2)
    finish_row(zz, 0)
    arrivals(2, 1)
    arrivals(2, 2)

    def step(s, last_down):
        arrivals(s, 0, last_down=last_down)
        relay_across(zrow(1 - s), 2 * s - 3)
        relay_across(zrow(s - 1), 2 * s - 2)
        finish_row(zrow(2 - s), 2 * s - 5)
        arrivals(s, 1, last_down=last_down)
        finish_row(zrow(s - 2), 2 * s - 4)
        arrivals(s, 2, last_down=last_down)

    @pl.loop(3, steps - 1)
    def _(s):
        step(s, False)

    step(steps - 1, True)

    arrivals(steps, 0, last_up=True, has_down=False)
    relay_across(zrow(1 - steps), 2 * steps - 3)
    relay_across(zrow(steps - 1), 2 * steps - 2)
    finish_row(zrow(2 - steps), 2 * steps - 5)
    relay_across(zrow(-steps), 2 * steps - 1)
    finish_row(zrow(steps - 2), 2 * steps - 4)
    finish_row(zrow(1 - steps), 2 * steps - 3)
    finish_row(zrow(steps - 1), 2 * steps - 2)
    arrivals(steps, 1, last_up=True, has_down=False)
    arrivals(steps, 2, last_up=True, has_down=False)
    finish_row(zrow(-steps), 2 * steps - 1)

    e_send = rcopy(acc.at[1 - core], accr, esem.at[0], esem.at[1], partner)
    e_send.start()
    local[9].wait()
    e_send.wait_recv()
    sums = jnp.sum(acc[core, HD:, :] + accr[HD:, :], axis=0, keepdims=True)
    attended = (acc[core, 0:HD, :] + accr[0:HD, :]) / sums
    attended = jnp.concatenate(
        [jnp.transpose(attended[:, h * HD:(h + 1) * HD]) for h in range(heads)], axis=1).astype(BF16)
    share = jnp.dot(attended, wo_v[...], preferred_element_type=F32)
    share = share.reshape(YN, BLK // YN, share.shape[1])
    mf[...] = share
    mbuf[...] = share.astype(BF16)
    m_sends = []
    for d in (1, 2, 3):
        m_sends.append(rcopy(
            mbuf.at[lax.rem(yy + d, YN)], rbuf.at[d - 1], y2send.at[d - 1], y2recv.at[d - 1], ypeer(d)))
    for copy in m_sends:
        copy.start()

    for d in (1, 2, 3):
        rcopy(nbuf.at[yy], nbuf.at[yy], ysend.at[d - 1], yrecv.at[d - 1], ypeer(d)).wait_send()
    for copy in a_sends:
        copy.wait_send()
    q_send.wait_send()
    e_send.wait_send()

    @pl.loop(0, steps)
    def _(s):
        for k in range(3):
            up(s, k).wait_send()

    @pl.loop(0, steps - 1)
    def _(s):
        for k in range(3):
            down(s, k).wait_send()

    @pl.loop(0, zn)
    def _(j):
        for i in range(4):
            across(zz, j, i).wait_send()

    total = mf[yy]
    for d in (1, 2, 3):
        m_sends[d - 1].wait_recv()
        total = total + rbuf[d - 1].astype(F32)
    out_ref[...] = total.astype(BF16)
    for copy in m_sends:
        copy.wait_send()


def per_device(sp, tokens, norm_gain, wq, wk, wv, query_gain, key_gain, wo):
    zn = sp // (2 * XN)
    steps = zn // 2
    rows, width = tokens.shape
    row_table, col_table = position_tables(sp)
    queries = wq.shape[1] // HD * BLK
    args = (
        tokens, norm_gain.reshape(1, -1), wq, wk, wv, query_gain.reshape(1, -1), key_gain.reshape(1, -1), wo,
        jnp.asarray(row_table), jnp.asarray(col_table),
    )
    DMA = pltpu.SemaphoreType.DMA
    scratch = [
        pltpu.VMEM(args[0].shape, BF16), pltpu.VMEM(args[1].shape, F32), pltpu.VMEM(wq.shape, BF16),
        pltpu.VMEM(wk.shape, BF16), pltpu.VMEM(wv.shape, BF16), pltpu.VMEM((1, HD), F32), pltpu.VMEM((1, HD), F32),
        pltpu.VMEM(wo.shape, BF16), pltpu.VMEM((8, HD), F32), pltpu.VMEM((2, BLK, HD), F32),
        pltpu.VMEM((YN, rows, width), BF16),
        pltpu.VMEM((zn, XN, 2 * BLK, HD), BF16),
        pltpu.VMEM((2, HD, queries), BF16),
        pltpu.VMEM((2, HD + 8, queries), F32),
        pltpu.VMEM((HD + 8, queries), F32),
        pltpu.VMEM((YN, rows, width), F32),
        pltpu.VMEM((YN, rows, width), BF16),
        pltpu.VMEM((YN - 1, rows, width), BF16),
        DMA((10,)), DMA((3,)), DMA((3,)), DMA((3,)), DMA((3,)), DMA((3,)), DMA((3,)),
        DMA((steps, 3)), DMA((steps + 1, 3)), DMA((steps - 1, 3)), DMA((steps, 3)),
        DMA((zn, 4)), DMA((zn, 4)), DMA((2,)), DMA((2,)),
    ]
    return pl.pallas_call(
        functools.partial(layer_kernel, zn),
        out_shape=jax.ShapeDtypeStruct((rows, width), BF16),
        in_specs=[pl.BlockSpec(memory_space=pltpu.HBM)] * len(args),
        out_specs=pl.BlockSpec(memory_space=pltpu.VMEM),
        scratch_shapes=scratch,
        compiler_params=pltpu.CompilerParams(
            collective_id=0, has_side_effects=True, vmem_limit_bytes=56 * 2**20),
        name="attention_layer",
    )(*args)


def solution(mesh):
    return jax.shard_map(
        functools.partial(per_device, mesh.shape["sp"]),
        mesh=mesh,
        in_specs=(
            P(("sp", "tp"), None), P(), P(None, "tp"), P(None, "tp"), P(None, "tp"), P(), P(), P("tp", None),
        ),
        out_specs=P(("sp", "tp"), None),
        check_vma=False,
    )
```
